32 devices in a mesh: grp: 2 (over x), tp: 16 (over z, y, core).
Axes of the slice: x: 2, y: 2, z: 4, core: 2. Of those that a mesh axis runs over, the one named last changes fastest.
Arguments:
- tokens: bfloat16 [3072, 2048], P('grp', 'tp'), parts along dimension 0, may hold values from -6 to 6
- lengths: int32 [192], P('grp'), parts along dimension 0, may hold values from 1 to 16, 960 in all
- gain_first: float32 [2048], replicated, may hold values from 0.1 to 1.9
- query_first: bfloat16 [2048, 1024], P(None, 'tp'), may hold values from -0.125 to 0.125
- key_first: bfloat16 [2048, 1024], P(None, 'tp'), may hold values from -0.125 to 0.125
- value_first: bfloat16 [2048, 2048], P(None, 'tp'), may hold values from -0.125 to 0.125
- gate_first: bfloat16 [2048, 2048], P(None, 'tp'), may hold values from -0.125 to 0.125
- out_first: bfloat16 [2048, 2048], P('tp'), may hold values from -0.1875 to 0.1875
- state_first: float32 [192, 16, 64, 128], P('grp', 'tp'), parts along dimension 0, may hold values from -0.9 to 0.9
- gain_second: float32 [2048], replicated, may hold values from 0.1 to 1.9
- query_second: bfloat16 [2048, 1024], P(None, 'tp'), may hold values from -0.125 to 0.125
- key_second: bfloat16 [2048, 1024], P(None, 'tp'), may hold values from -0.125 to 0.125
- value_second: bfloat16 [2048, 2048], P(None, 'tp'), may hold values from -0.125 to 0.125
- gate_second: bfloat16 [2048, 2048], P(None, 'tp'), may hold values from -0.125 to 0.125
- out_second: bfloat16 [2048, 2048], P('tp'), may hold values from -0.1875 to 0.1875
- state_second: float32 [192, 16, 64, 128], P('grp', 'tp'), parts along dimension 0, may hold values from -0.9 to 0.9
Outputs:
- mixed_out: bfloat16 [3072, 2048], P('grp', 'tp'), parts along dimension 0
- state_first_new: float32 [192, 16, 64, 128], P('grp', 'tp'), parts along dimension 0
- state_second_new: float32 [192, 16, 64, 128], P('grp', 'tp'), parts along dimension 0
The draws below stay inside these ranges and needn't reach their ends.
There are 2 independent parts, one for each index of `grp`. The reference program is written for one: setup_inputs(seed, part) draws one part's arguments, and reference() takes and returns one part's arrays. A program takes and returns all parts, laid end to end along the dimension named above; an argument that names none is the same for every part. Nothing has to cross between parts.
All inputs are finite; a program needn't handle non-finite values.
Results may differ from the reference program's by a relative error of at most 0.025.
Values may be sent and summed in bfloat16 or wider, within the bound.
A program may use at most 128 MiB of HBM per device.

```python
import math
import jax
import jax.numpy as jnp
import numpy as np
from jax import lax

D = 2048
DK = 64
DV = 128
HEADS = 16
BATCH = 96
BLOCK = 16
PAST_LEN = 16384
ROWS = 1536
LIVE_TOTAL = 960


def raised(values, key, source, target, shards_of, factor):
    owner, partner = [(jnp.arange(values.shape[axis_at]) // (values.shape[axis_at] // shards_of)).reshape([-1 if axis == axis_at else 1 for axis in range(values.ndim)]) for axis_at in (source, target)]
    chosen = jax.random.permutation(key, shards_of)[partner]
    strong = (owner == chosen) | (owner == (partner + shards_of // 2) % shards_of)
    return jnp.where(strong, factor * values, values)


def steps_of(stream_key, dims, shards, least, largest):
    def one(position, blocks):
        steps = jax.random.uniform(jax.random.fold_in(jax.random.fold_in(stream_key, 6), position), (blocks,), jnp.float32, least / len(shards), largest / len(shards))
        return jnp.repeat(jnp.exp(steps), dims[position] // blocks).reshape((-1,) + (1,) * (len(dims) - position - 1))

    factor_of = one(*shards[0])
    for cut in shards[1:]:
        factor_of = factor_of * one(*cut)
    return factor_of


def profile(number_of, total, bound, lean):
    loads = [(1 << 20) // math.isqrt(rank ** lean) + 1 for rank in range(2, number_of + 1)]
    rest, given = total - bound - (number_of - 1), [1] * (number_of - 1)
    while rest > 0:
        candidates = [i for i in range(number_of - 1) if given[i] < bound]
        whole, remaining = sum([loads[i] for i in candidates]), rest
        for i in candidates:
            extra = min(bound - given[i], max(1, remaining * loads[i] // whole), rest)
            given[i] = given[i] + extra
            rest = rest - extra
    return np.array([bound] + given)


def ragged_sizes(key, number_of, total, most, slope):
    if number_of == 2:
        one = jax.random.randint(key, (), max(1, total - most), min(most, total - 1) + 1)
        return jnp.stack([one, total - one])
    sizes = jnp.asarray(profile(number_of, total, most, slope), jnp.int32)
    couples = (number_of - 1) // 2
    giver, taker = sizes[1:1 + 2 * couples:2], sizes[2:2 + 2 * couples:2]
    margin = jnp.minimum(giver - 1, most - taker)
    shifted = jax.random.randint(jax.random.fold_in(key, 1), (couples,), 0, 1 << 20) % (margin + 1)
    sizes = sizes.at[1:1 + 2 * couples:2].set(giver - shifted).at[2:2 + 2 * couples:2].set(taker + shifted)
    return sizes[jax.random.permutation(jax.random.fold_in(key, 2), number_of)]


def centred(key, dims, spread, reach, cuts=(), held_as=jnp.bfloat16):
    values = jax.random.normal(key, dims, jnp.float32) * spread
    if len(cuts) > 0:
        values = steps_of(key, dims, cuts, -0.22, 0.18) * values
    return jnp.clip(values, min=-reach, max=reach).astype(held_as)


def heavy_noise(rng, dims, scale, most, pieces, heavy, kind=jnp.bfloat16):
    entries = scale * jax.random.normal(rng, dims, jnp.float32)
    if pieces:
        entries = entries * steps_of(rng, dims, pieces, -0.22, 0.18)
    return jnp.clip(raised(entries, jax.random.fold_in(rng, 3), *heavy), -most, most).astype(kind)


def setup_inputs(seed: int = 0, part: int = 0) -> dict:
    key_of = jax.random.split(jax.random.key(seed), 17)
    own_keys = jax.random.split(jax.random.fold_in(key_of[16], part), 17)
    return {
        "tokens": centred(own_keys[0], (ROWS, D), 1.0, 6.0, ((1, 16),)),
        "lengths": ragged_sizes(own_keys[1], BATCH, LIVE_TOTAL, BLOCK, 2).astype(jnp.int32),
        "gain_first": jnp.clip(1.0 + 0.18 * jax.random.normal(key_of[2], (D,), jnp.float32), 0.1, 1.9),
        "query_first": centred(key_of[3], (D, HEADS * DK), D ** -0.5, 0.125, ((1, 16),)),
        "key_first": centred(key_of[4], (D, HEADS * DK), D ** -0.5, 0.125, ((1, 16),)),
        "value_first": centred(key_of[5], (D, HEADS * DV), D ** -0.5, 0.125, ((1, 16),)),
        "gate_first": centred(key_of[6], (D, HEADS * DV), D ** -0.5, 0.125, ((1, 16),)),
        "out_first": heavy_noise(key_of[7], (HEADS * DV, D), (HEADS * DV) ** -0.5, 0.1875, ((0, 16),), (0, 1, 16, 2.0)),
        "state_first": centred(own_keys[8], (BATCH, HEADS, DK, DV), 0.15, 0.9, ((1, 16),), jnp.float32),
        "gain_second": jnp.clip(1.0 + 0.18 * jax.random.normal(key_of[9], (D,), jnp.float32), 0.1, 1.9),
        "query_second": centred(key_of[10], (D, HEADS * DK), D ** -0.5, 0.125, ((1, 16),)),
        "key_second": centred(key_of[11], (D, HEADS * DK), D ** -0.5, 0.125, ((1, 16),)),
        "value_second": centred(key_of[12], (D, HEADS * DV), D ** -0.5, 0.125, ((1, 16),)),
        "gate_second": centred(key_of[13], (D, HEADS * DV), D ** -0.5, 0.125, ((1, 16),)),
        "out_second": heavy_noise(key_of[14], (HEADS * DV, D), (HEADS * DV) ** -0.5, 0.1875, ((0, 16),), (0, 1, 16, 2.0)),
        "state_second": centred(own_keys[15], (BATCH, HEADS, DK, DV), 0.15, 0.9, ((1, 16),), jnp.float32),
    }


NORM_EPSILON = 1e-06
ROPE_BASE = 10000.0

def norm_rows(rows_in, gain_vec):
    rows_f = rows_in.astype(jnp.float32)
    inv_rms = lax.rsqrt(lax.optimization_barrier(jnp.mean(rows_f * rows_f, axis=-1, keepdims=True)) + NORM_EPSILON)
    return (rows_f * inv_rms * gain_vec.astype(jnp.float32)).astype(jnp.bfloat16)

def rotate(vectors):
    half_dim = vectors.shape[-1] // 2
    inverse = ROPE_BASE ** (-jnp.arange(half_dim, dtype=jnp.float32) / half_dim)
    positions = PAST_LEN + jnp.arange(vectors.shape[1], dtype=jnp.float32)
    angles = positions[:, None] * inverse[None, :]
    cosine_table = jnp.cos(angles)[None, :, None, :]
    sine_table = jnp.sin(angles)[None, :, None, :]
    front_half = vectors[..., :half_dim]
    back_half = vectors[..., half_dim:]
    return jnp.concatenate([front_half * cosine_table - back_half * sine_table, front_half * sine_table + back_half * cosine_table], axis=-1)

def decay_logs(head_total):
    head_ids = jnp.arange(head_total).astype(jnp.float32)
    return jnp.log(1.0 - 2.0 ** (-1.5 - 6.0 * head_ids / (head_total - 1)))

def retain(normed, lengths, w_query, w_key, w_value, w_gate, state_in, log_gamma):
    batch_size, head_count, key_dim, value_dim = state_in.shape
    block_len = normed.shape[0] // batch_size
    queries = jnp.dot(normed, w_query, preferred_element_type=jnp.float32)
    queries = rotate(queries.reshape(batch_size, block_len, head_count, key_dim)).astype(jnp.bfloat16)
    key_rows = jnp.dot(normed, w_key, preferred_element_type=jnp.float32)
    key_rows = (rotate(key_rows.reshape(batch_size, block_len, head_count, key_dim)) * key_dim ** (-0.5)).astype(jnp.bfloat16)
    values = jnp.dot(normed, w_value, preferred_element_type=jnp.float32).astype(jnp.bfloat16)
    values = values.reshape(batch_size, block_len, head_count, value_dim)
    gate_pre = jnp.dot(normed, w_gate, preferred_element_type=jnp.float32).reshape(batch_size, block_len, head_count, value_dim)
    slot_ids = jnp.arange(block_len).astype(jnp.float32)
    live_count = lengths.astype(jnp.float32)
    active = (slot_ids[None, :] < live_count[:, None]).astype(jnp.float32)
    step_gap = slot_ids[:, None] - slot_ids[None, :]
    causal = (step_gap >= 0.0).astype(jnp.float32)
    within = jnp.exp(log_gamma[:, None, None] * jnp.maximum(step_gap, 0.0)[None]) * causal[None]
    scores = jnp.einsum('bihd,bjhd->bhij', queries.astype(jnp.float32), key_rows.astype(jnp.float32))
    weights = (scores * within[None]).astype(jnp.bfloat16)
    inner_part = jnp.einsum('bhij,bjhe->bihe', weights.astype(jnp.float32), values.astype(jnp.float32))
    carried = jnp.einsum('bihd,bhde->bihe', queries.astype(jnp.float32), state_in, precision=lax.Precision.HIGHEST)
    carried = carried * jnp.exp(log_gamma[None, None, :] * (slot_ids[None, :, None] + 1.0))[..., None]
    retained = (inner_part + carried) * active[:, :, None, None]
    lead_gap = live_count[:, None] - 1.0 - slot_ids[None, :]
    key_weight = jnp.exp(log_gamma[None, None, :] * jnp.maximum(lead_gap, 0.0)[:, :, None]) * active[:, :, None]
    added_state = jnp.einsum('bjhd,bjhe->bhde', key_rows.astype(jnp.float32) * key_weight[..., None], values.astype(jnp.float32), precision=lax.Precision.HIGHEST)
    new_state = state_in * jnp.exp(log_gamma[None, :] * live_count[:, None])[:, :, None, None] + added_state
    inv_rms = lax.rsqrt(lax.optimization_barrier(jnp.mean(retained * retained, axis=-1, keepdims=True)) + NORM_EPSILON)
    heads_out = (retained * inv_rms * jax.nn.silu(gate_pre)).astype(jnp.bfloat16)
    return (heads_out.reshape(batch_size * block_len, head_count * value_dim), new_state)

def one_block(stream, lengths, gain_vec, w_query, w_key, w_value, w_gate, w_out, state_in):
    normed = norm_rows(stream, gain_vec)
    log_gamma = decay_logs(state_in.shape[1])
    heads_out, new_state = retain(normed, lengths, w_query, w_key, w_value, w_gate, state_in, log_gamma)
    mix_rows = jnp.dot(heads_out, w_out, preferred_element_type=jnp.float32).astype(jnp.bfloat16)
    result = (stream.astype(jnp.float32) + mix_rows.astype(jnp.float32)).astype(jnp.bfloat16)
    return (result, new_state)

def reference(tokens, lengths, gain_first, query_first, key_first, value_first, gate_first, out_first, state_first, gain_second, query_second, key_second, value_second, gate_second, out_second, state_second):
    middle, state_first_new = one_block(tokens, lengths, gain_first, query_first, key_first, value_first, gate_first, out_first, state_first)
    mixed_out, state_second_new = one_block(middle, lengths, gain_second, query_second, key_second, value_second, gate_second, out_second, state_second)
    return (mixed_out, state_first_new, state_second_new)
```

```python
import functools

import jax
import jax.numpy as jnp
from jax import lax
from jax.experimental import pallas as pl
from jax.experimental.pallas import tpu as pltpu
from jax.sharding import PartitionSpec as P

PAST_LEN = 16384
LIVE_TOTAL = 960

NORM_EPSILON = 1e-06
ROPE_BASE = 10000.0

MESH = pl.DeviceIdType.MESH
F32 = jnp.float32
BF16 = jnp.bfloat16


def decay_logs(head_count):
    head_total = lax.axis_size("tp") * head_count
    head_ids = (lax.axis_index("tp") * head_count + jnp.arange(head_count)).astype(F32)
    return jnp.log(1.0 - 2.0 ** (-1.5 - 6.0 * head_ids / (head_total - 1)))


def rope_tables(block_len, key_dim):
    half_dim = key_dim // 2
    inverse = ROPE_BASE ** (-jnp.arange(half_dim, dtype=F32) / half_dim)
    positions = PAST_LEN + jnp.arange(block_len, dtype=F32)
    angles = positions[:, None] * inverse[None, :]
    cosines, sines = jnp.cos(angles), jnp.sin(angles)
    cosines = jnp.concatenate([cosines, cosines], axis=1)
    sines = jnp.concatenate([-sines, sines], axis=1)
    scale = key_dim ** (-0.5)
    return jnp.concatenate([cosines, cosines * scale, sines, sines * scale], axis=1)


def retain(qkv, lengths, state_in):
    batch_size, head_count, key_dim, value_dim = state_in.shape
    block_len = qkv.shape[0] // batch_size
    log_gamma = decay_logs(head_count)
    queries = qkv[:, :key_dim].reshape(batch_size, block_len, 1, key_dim)
    key_rows = qkv[:, key_dim : 2 * key_dim].reshape(batch_size, block_len, 1, key_dim)
    values = qkv[:, 2 * key_dim :].reshape(batch_size, block_len, 1, value_dim)
    slot_ids = jnp.arange(block_len).astype(F32)
    live_count = lengths.astype(F32)
    active = (slot_ids[None, :] < live_count[:, None]).astype(F32)
    step_gap = slot_ids[:, None] - slot_ids[None, :]
    causal = (step_gap >= 0.0).astype(F32)
    within = jnp.exp(log_gamma[:, None, None] * jnp.maximum(step_gap, 0.0)[None]) * causal[None]
    scores = jnp.einsum("bihd,bjhd->bhij", queries, key_rows, preferred_element_type=F32)
    weights = (scores * within[None]).astype(BF16)
    inner_part = jnp.einsum("bhij,bjhe->bihe", weights, values, preferred_element_type=F32)
    carried = jnp.einsum(
        "bihd,bhde->bihe", queries.astype(F32), state_in, precision=lax.Precision.HIGHEST
    )
    carried = (
        carried * jnp.exp(log_gamma[None, None, :] * (slot_ids[None, :, None] + 1.0))[..., None]
    )
    retained = (inner_part + carried) * active[:, :, None, None]
    lead_gap = live_count[:, None] - 1.0 - slot_ids[None, :]
    key_weight = (
        jnp.exp(log_gamma[None, None, :] * jnp.maximum(lead_gap, 0.0)[:, :, None])
        * active[:, :, None]
    )
    added_state = jnp.einsum(
        "bjhd,bjhe->bhde",
        key_rows.astype(F32) * key_weight[..., None],
        values.astype(F32),
        precision=lax.Precision.HIGHEST,
    )
    new_state = (
        state_in * jnp.exp(log_gamma[None, :] * live_count[:, None])[:, :, None, None] + added_state
    )
    inv_rms = lax.rsqrt(jnp.mean(retained * retained, axis=-1, keepdims=True) + NORM_EPSILON)
    normed = (retained * inv_rms).astype(BF16)
    return normed.reshape(batch_size * block_len, value_dim), new_state


class Ring:
    def __init__(self, n, rows, pieces):
        self.n, self.m = n, n // 2
        self.rows, self.pieces = rows, pieces
        self.size = rows // pieces
        me = lax.axis_index("tp")
        self.core = lax.rem(me, 2)
        chip = lax.div(me, 2)
        odd = lax.rem(chip, 2)
        half = lax.div(chip, 2)
        self.pos = (1 - odd) * half + odd * (self.m - 1 - half)
        self.me = me
        self.partner = chip * 2 + 1 - self.core
        self.right = self.device(self.pos + 1)
        self.left = self.device(self.pos - 1)

    def device(self, pos, other=False):
        m = self.m
        pos = lax.rem(pos + m, m)
        far = lax.div(pos, (m + 1) // 2)
        chip = (1 - far) * 2 * pos + far * (2 * (m - 1 - pos) + 1)
        return chip * 2 + (1 - self.core if other else self.core)

    def enter(self):
        barrier = pltpu.get_barrier_semaphore()
        for device in (self.left, self.right, self.partner):
            pl.semaphore_signal(barrier, inc=1, device_id={"tp": device}, device_id_type=MESH)
        pl.semaphore_wait(barrier, 3)

    def piece(self, j):
        return pl.ds(j * self.size, self.size)

    def clockwise(self, j):
        return j < self.pieces // 2

    def to(self, j):
        return self.right if self.clockwise(j) else self.left

    def back(self, j, steps):
        return self.pos - steps if self.clockwise(j) else self.pos + steps

    def order(self):
        half = self.pieces // 2
        return [j for pair in range(half) for j in (pair, pair + half)]


def remote(src, dst, send, recv, device):
    return pltpu.make_async_remote_copy(
        src_ref=src,
        dst_ref=dst,
        send_sem=send,
        recv_sem=recv,
        device_id={"tp": device},
        device_id_type=MESH,
    )


def gather_stage(ring, own_ref, whole, sems):
    width = own_ref.shape[1]
    send, recv, share_send, share_recv = sems

    def columns(device):
        return pl.ds(pl.multiple_of(device * width, width), width)

    whole[:, columns(ring.me)] = own_ref[...]
    hops, shares = {}, []
    for s in range(ring.m):
        for j in ring.order():
            rows = ring.piece(j)
            cols = columns(ring.device(ring.back(j, s)))
            if s > 0:
                hops[j, s - 1].wait_recv()
            src = own_ref.at[rows, :] if s == 0 else whole.at[rows, cols]
            if s < ring.m - 1:
                hop = remote(src, whole.at[rows, cols], send.at[j, s], recv.at[j, s], ring.to(j))
                hop.start()
                hops[j, s] = hop
            share = remote(
                src, whole.at[rows, cols], share_send.at[j, s], share_recv.at[j, s], ring.partner
            )
            share.start()
            shares.append(share)
    for hop in hops.values():
        hop.wait_send()
    for share in shares:
        share.wait()


def fill_weights(wq_ref, wk_ref, wv_ref, wg_ref, wcat):
    at = 0
    for ref in (wq_ref, wk_ref, wv_ref, wg_ref):
        wcat[:, at : at + ref.shape[1]] = ref[...]
        at += ref.shape[1]


def project_stage(whole, gain_ref, wcat, table_ref, qkv_ref, gate_ref, key_dim):
    rows, width = whole.shape
    tile = 16

    @pl.loop(0, rows // tile)
    def _(i):
        at = pl.ds(pl.multiple_of(i * tile, tile), tile)
        x = whole[at, :].astype(F32)
        inv = lax.rsqrt(jnp.mean(x * x, axis=-1, keepdims=True) + NORM_EPSILON)
        whole[at, :] = (x * inv * gain_ref[...]).astype(BF16)

    both = 2 * key_dim
    value_dim = gate_ref.shape[1]
    block = rows // 4

    @pl.loop(0, 4)
    def _(i):
        at = pl.ds(pl.multiple_of(i * block, block), block)
        out = jnp.dot(whole[at, :], wcat[...], preferred_element_type=F32)
        qk = out[:, :both]
        lane = lax.broadcasted_iota(jnp.int32, qk.shape, 1)
        ahead = pltpu.roll(qk, both - key_dim // 2, 1)
        behind = pltpu.roll(qk, key_dim // 2, 1)
        swapped = jnp.where(lax.rem(lane, key_dim) < key_dim // 2, ahead, behind)
        turned = qk * table_ref[at, :both] + swapped * table_ref[at, both:]
        qkv_ref[at, :both] = turned.astype(BF16)
        qkv_ref[at, both:] = out[:, both : both + value_dim].astype(BF16)
        gate = out[:, both + value_dim :]
        gate_ref[at, :] = gate / (1.0 + jnp.exp(-gate))


def scatter_stage(ring, h_ref, w_ref, x_ref, out_ref, h_pair, w_pair, outbox, inbox, sems):
    width = x_ref.shape[1]
    depth = h_ref.shape[1]
    send, recv, pair_send, pair_recv = sems
    w_copy = remote(
        w_ref, w_pair.at[pl.ds(depth, depth), :], pair_send.at[0], pair_recv.at[0], ring.partner
    )
    w_copy.start()
    h_copy = remote(
        h_ref, h_pair.at[:, pl.ds(depth, depth)], pair_send.at[1], pair_recv.at[1], ring.partner
    )
    h_copy.start()
    w_pair[:depth, :] = w_ref[...]
    h_pair[:, :depth] = h_ref[...]
    w_copy.wait()
    h_copy.wait()
    hops = {}
    for s in range(ring.m):
        for j in ring.order():
            rows = ring.piece(j)
            target = ring.device(ring.back(j, s + 1))
            cols = pl.ds(pl.multiple_of(target * width, width), width)
            part = jnp.dot(h_pair[rows, :], w_pair[:, cols], preferred_element_type=F32)
            if s > 0:
                hops[j, s - 1].wait_recv()
                part = part + inbox[j, s - 1].astype(F32)
            if s < ring.m - 1:
                outbox[j, s] = part.astype(BF16)
                hop = remote(
                    outbox.at[j, s], inbox.at[j, s], send.at[j, s], recv.at[j, s], ring.to(j)
                )
                hop.start()
                hops[j, s] = hop
            else:
                mix = part.astype(BF16).astype(F32)
                out_ref[rows, :] = (x_ref[rows, :].astype(F32) + mix).astype(BF16)
    for hop in hops.values():
        hop.wait_send()


def first_kernel(n, pieces, key_dim, *refs):
    x_ref, gain_ref, wq, wk, wv, wg, table, qkv, gate, whole, wcat, *sems = refs
    ring = Ring(n, x_ref.shape[0], pieces)
    ring.enter()
    fill_weights(wq, wk, wv, wg, wcat)
    gather_stage(ring, x_ref, whole, sems)
    project_stage(whole, gain_ref, wcat, table, qkv, gate, key_dim)


def middle_kernel(n, pieces, key_dim, *refs):
    h_ref, w_ref, x_ref, gain_ref, wq, wk, wv, wg, table = refs[:9]
    x1, qkv, gate, whole, wcat, h_pair, w_pair, outbox, inbox = refs[9:18]
    sems = refs[18:]
    ring = Ring(n, x_ref.shape[0], pieces)
    ring.enter()
    fill_weights(wq, wk, wv, wg, wcat)
    scatter_stage(ring, h_ref, w_ref, x_ref, x1, h_pair, w_pair, outbox, inbox, sems[4:])
    gather_stage(ring, x1, whole, sems[:4])
    project_stage(whole, gain_ref, wcat, table, qkv, gate, key_dim)


def last_kernel(n, pieces, *refs):
    h_ref, w_ref, x_ref, out_ref, h_pair, w_pair, outbox, inbox, *sems = refs
    ring = Ring(n, x_ref.shape[0], pieces)
    ring.enter()
    scatter_stage(ring, h_ref, w_ref, x_ref, out_ref, h_pair, w_pair, outbox, inbox, sems)


def gather_scratch(n, pieces, rows, width, wide):
    scratch = [pltpu.VMEM((rows, n * width), BF16), pltpu.VMEM((n * width, wide), BF16)]
    m = n // 2
    sems = [pltpu.SemaphoreType.DMA((pieces, m - 1))] * 2 + [pltpu.SemaphoreType.DMA((pieces, m))] * 2
    return scratch, sems


def scatter_scratch(n, pieces, rows, width, depth):
    m = n // 2
    boxes = pltpu.VMEM((pieces, m - 1, rows // pieces, width), BF16)
    scratch = [
        pltpu.VMEM((rows, 2 * depth), BF16),
        pltpu.VMEM((2 * depth, n * width), BF16),
        boxes,
        boxes,
    ]
    sems = [pltpu.SemaphoreType.DMA((pieces, m - 1))] * 2 + [pltpu.SemaphoreType.DMA((2,))] * 2
    return scratch, sems


def call(kernel, outs, scratch, collective_id, *args):
    vmem = pl.BlockSpec(memory_space=pltpu.VMEM)
    return pl.pallas_call(
        kernel,
        out_shape=outs,
        in_specs=[vmem] * len(args),
        out_specs=[vmem] * len(outs),
        scratch_shapes=scratch,
        compiler_params=pltpu.CompilerParams(
            collective_id=collective_id, has_side_effects=True, vmem_limit_bytes=56 * 2**20
        ),
    )(*args)


def plain_project(x, gain, weights, table, key_dim):
    whole = lax.all_gather(x, "tp", axis=1, tiled=True).astype(F32)
    inv = lax.rsqrt(jnp.mean(whole * whole, axis=-1, keepdims=True) + NORM_EPSILON)
    normed = (whole * inv * gain).astype(BF16)
    qk = jnp.dot(normed, jnp.concatenate(weights[:2], axis=1), preferred_element_type=F32)
    halves = qk.reshape(qk.shape[0], 2, 2, key_dim // 2)
    swapped = halves[:, :, ::-1].reshape(qk.shape)
    turned = qk * table[:, : 2 * key_dim] + swapped * table[:, 2 * key_dim :]
    values = jnp.dot(normed, weights[2], preferred_element_type=F32)
    gate = jnp.dot(normed, weights[3], preferred_element_type=F32)
    qkv = jnp.concatenate([turned.astype(BF16), values.astype(BF16)], axis=1)
    return qkv, jax.nn.silu(gate)


def plain_finish(h, w_out, x):
    part = jnp.dot(h, w_out, preferred_element_type=F32).astype(BF16)
    mix = lax.psum_scatter(part, "tp", scatter_dimension=1, tiled=True)
    return (x.astype(F32) + mix.astype(F32)).astype(BF16)


def shards(
    tokens,
    lengths,
    gain_first,
    query_first,
    key_first,
    value_first,
    gate_first,
    out_first,
    state_first,
    gain_second,
    query_second,
    key_second,
    value_second,
    gate_second,
    out_second,
    state_second,
):
    n = lax.axis_size("tp")
    batch_size, head_count, key_dim, value_dim = state_first.shape
    slots, width = tokens.shape
    block_len = slots // batch_size
    rows = LIVE_TOTAL

    lengths_i = lengths.astype(jnp.int32)
    starts = jnp.cumsum(lengths_i) - lengths_i
    slot = jnp.arange(block_len, dtype=jnp.int32)
    live = slot[None, :] < lengths_i[:, None]
    target = jnp.where(live, starts[:, None] + slot[None, :], -1).reshape(slots)
    pack = (jnp.arange(rows, dtype=jnp.int32)[:, None] == target[None, :]).astype(BF16)

    def packed(padded):
        return jnp.dot(pack, padded, preferred_element_type=F32)

    def spread(rows_in):
        return lax.dot_general(
            pack, rows_in, (((0,), (0,)), ((), ())), preferred_element_type=F32
        ).astype(rows_in.dtype)

    slot_hot = jnp.tile(jnp.eye(block_len, dtype=BF16), (batch_size, 1))
    table = jnp.dot(
        packed(slot_hot), rope_tables(block_len, key_dim), precision=lax.Precision.HIGHEST
    )
    x = packed(tokens).astype(BF16)

    weights_first = (query_first, key_first, value_first, gate_first)
    weights_second = (query_second, key_second, value_second, gate_second)
    wide = sum(w.shape[1] for w in weights_first)
    pieces = next((p for p in (6, 4, 2) if rows % (16 * p) == 0), 0)
    ringed = (
        n >= 4
        and n % 2 == 0
        and pieces > 0
        and rows % 64 == 0
        and head_count == 1
        and width % 128 == 0
        and value_dim % 128 == 0
        and 2 * key_dim % 128 == 0
    )
    outs = [
        jax.ShapeDtypeStruct((rows, 2 * key_dim + value_dim), BF16),
        jax.ShapeDtypeStruct((rows, value_dim), F32),
    ]
    own = jax.ShapeDtypeStruct((rows, width), BF16)
    gather_bufs, gather_sems = gather_scratch(n, pieces or 2, rows, width, wide)
    scatter_bufs, scatter_sems = scatter_scratch(n, pieces or 2, rows, width, value_dim)

    if ringed:
        qkv, gate = call(
            functools.partial(first_kernel, n, pieces, key_dim),
            outs,
            gather_bufs + gather_sems,
            0,
            x,
            gain_first[None],
            *weights_first,
            table,
        )
    else:
        qkv, gate = plain_project(x, gain_first, weights_first, table, key_dim)
    normed, state_first_new = retain(spread(qkv), lengths, state_first)
    h = (packed(normed) * gate).astype(BF16)
    if ringed:
        x1, qkv, gate = call(
            functools.partial(middle_kernel, n, pieces, key_dim),
            [own] + outs,
            gather_bufs + scatter_bufs + gather_sems + scatter_sems,
            1,
            h,
            out_first,
            x,
            gain_second[None],
            *weights_second,
            table,
        )
    else:
        x1 = plain_finish(h, out_first, x)
        qkv, gate = plain_project(x1, gain_second, weights_second, table, key_dim)
    normed, state_second_new = retain(spread(qkv), lengths, state_second)
    h = (packed(normed) * gate).astype(BF16)
    if ringed:
        (y,) = call(
            functools.partial(last_kernel, n, pieces),
            [own],
            scatter_bufs + scatter_sems,
            2,
            h,
            out_second,
            x1,
        )
    else:
        y = plain_finish(h, out_second, x1)
    mixed_out = jnp.where(live.reshape(slots, 1), spread(y), tokens)
    return (mixed_out, state_first_new, state_second_new)


def solution(mesh):
    heads = P(None, "tp")
    state = P("grp", "tp", None, None)
    block = (P(), heads, heads, heads, heads, P("tp", None), state)
    in_specs = (P("grp", "tp"), P("grp")) + block + block
    out_specs = (P("grp", "tp"), state, state)
    return jax.shard_map(shards, mesh=mesh, in_specs=in_specs, out_specs=out_specs, check_vma=False)
```

```python
import functools

import jax
import jax.numpy as jnp
from jax import lax
from jax.experimental import pallas as pl
from jax.experimental.pallas import tpu as pltpu
from jax.sharding import PartitionSpec as P

PAST_LEN = 16384
LIVE_TOTAL = 960

NORM_EPSILON = 1e-06
ROPE_BASE = 10000.0

MESH = pl.DeviceIdType.MESH
F32 = jnp.float32
BF16 = jnp.bfloat16


def decay_logs(head_count):
    head_total = lax.axis_size("tp") * head_count
    head_ids = (lax.axis_index("tp") * head_count + jnp.arange(head_count)).astype(F32)
    return jnp.log(1.0 - 2.0 ** (-1.5 - 6.0 * head_ids / (head_total - 1)))


def rope_tables(block_len, key_dim):
    half_dim = key_dim // 2
    inverse = ROPE_BASE ** (-jnp.arange(half_dim, dtype=F32) / half_dim)
    positions = PAST_LEN + jnp.arange(block_len, dtype=F32)
    angles = positions[:, None] * inverse[None, :]
    cosines, sines = jnp.cos(angles), jnp.sin(angles)
    cosines = jnp.concatenate([cosines, cosines], axis=1)
    sines = jnp.concatenate([-sines, sines], axis=1)
    scale = key_dim ** (-0.5)
    return jnp.concatenate([cosines, cosines * scale, sines, sines * scale], axis=1)


def retain(qkv, lengths, state_in):
    batch_size, head_count, key_dim, value_dim = state_in.shape
    block_len = qkv.shape[0] // batch_size
    log_gamma = decay_logs(head_count)
    queries = qkv[:, :key_dim].reshape(batch_size, block_len, 1, key_dim)
    key_rows = qkv[:, key_dim : 2 * key_dim].reshape(batch_size, block_len, 1, key_dim)
    values = qkv[:, 2 * key_dim :].reshape(batch_size, block_len, 1, value_dim)
    slot_ids = jnp.arange(block_len).astype(F32)
    live_count = lengths.astype(F32)
    active = (slot_ids[None, :] < live_count[:, None]).astype(F32)
    step_gap = slot_ids[:, None] - slot_ids[None, :]
    causal = (step_gap >= 0.0).astype(F32)
    within = jnp.exp(log_gamma[:, None, None] * jnp.maximum(step_gap, 0.0)[None]) * causal[None]
    scores = jnp.einsum("bihd,bjhd->bhij", queries, key_rows, preferred_element_type=F32)
    weights = (scores * within[None]).astype(BF16)
    inner_part = jnp.einsum("bhij,bjhe->bihe", weights, values, preferred_element_type=F32)
    carried = jnp.einsum(
        "bihd,bhde->bihe", queries.astype(F32), state_in, precision=lax.Precision.HIGHEST
    )
    carried = (
        carried * jnp.exp(log_gamma[None, None, :] * (slot_ids[None, :, None] + 1.0))[..., None]
    )
    retained = (inner_part + carried) * active[:, :, None, None]
    lead_gap = live_count[:, None] - 1.0 - slot_ids[None, :]
    key_weight = (
        jnp.exp(log_gamma[None, None, :] * jnp.maximum(lead_gap, 0.0)[:, :, None])
        * active[:, :, None]
    )
    added_state = jnp.einsum(
        "bjhd,bjhe->bhde",
        key_rows.astype(F32) * key_weight[..., None],
        values.astype(F32),
        precision=lax.Precision.HIGHEST,
    )
    new_state = (
        state_in * jnp.exp(log_gamma[None, :] * live_count[:, None])[:, :, None, None] + added_state
    )
    inv_rms = lax.rsqrt(jnp.mean(retained * retained, axis=-1, keepdims=True) + NORM_EPSILON)
    normed = (retained * inv_rms).astype(BF16)
    return normed.reshape(batch_size * block_len, value_dim), new_state


def retention_kernel(key_dim, block_len, *refs):
    decay, side_ref, row_ref, within_ref, qkv_ref, gate_ref, state_ref = refs[:7]
    h_ref, new_ref, total = refs[7:]
    i = pl.program_id(0)
    rows = qkv_ref.shape[0]
    both = 2 * key_dim
    size = side_ref.shape[0]
    group = size // block_len
    side = side_ref[...]

    slots = lax.broadcasted_iota(jnp.int32, (size, rows), 1)
    hot = jnp.where(slots == side[:, 0:1].astype(jnp.int32), 1.0, 0.0).astype(BF16)
    padded = jnp.dot(hot, qkv_ref[...], preferred_element_type=F32)
    qk, values = padded[:, :both], padded[:, both:].astype(BF16)
    front = lax.broadcasted_iota(jnp.int32, qk.shape, 1) < key_dim
    turned = pltpu.roll(qk, key_dim, 1)
    queries, keys = jnp.where(front, qk, turned), jnp.where(front, turned, qk)
    scores = lax.dot_general(
        jnp.where(front, qk, 0.0).astype(BF16),
        keys.astype(BF16),
        (((1,), (1,)), ((), ())),
        preferred_element_type=F32,
    )
    weights = (scores * within_ref[...]).astype(BF16)
    retained = jnp.dot(weights, values, preferred_element_type=F32)

    wide = (size, group * key_dim)
    own = lax.div(lax.broadcasted_iota(jnp.int32, wide, 0), block_len) == lax.div(
        lax.broadcasted_iota(jnp.int32, wide, 1), key_dim
    )

    def per_sequence(doubled):
        spread = jnp.concatenate([doubled] * (group // 2), axis=1)
        return jnp.where(own, spread, 0.0).astype(BF16)

    state = state_ref[...].reshape(group * key_dim, state_ref.shape[-1])
    high = state.astype(BF16)
    low = (state - high.astype(F32)).astype(BF16)
    wide_q = per_sequence(queries)
    carried = jnp.dot(wide_q, high, preferred_element_type=F32)
    carried = carried + jnp.dot(wide_q, low, preferred_element_type=F32)
    retained = retained + carried * side[:, 1:2]
    inv = lax.rsqrt(jnp.mean(retained * retained, axis=-1, keepdims=True) + NORM_EPSILON)
    normed = (retained * inv).astype(BF16)
    places = lax.broadcasted_iota(jnp.int32, (rows, size), 0)
    back = jnp.where(places == row_ref[...], 1.0, 0.0).astype(BF16)
    part = jnp.dot(back, normed, preferred_element_type=F32)

    @pl.when(i == 0)
    def _():
        total[...] = part

    @pl.when(i > 0)
    def _():
        total[...] += part

    scaled = keys * side[:, 2:3]
    k_high = scaled.astype(BF16).astype(F32)
    added = None
    for piece in (k_high, scaled - k_high):
        term = lax.dot_general(
            per_sequence(piece), values, (((0,), (0,)), ((), ())), preferred_element_type=F32
        )
        added = term if added is None else added + term
    for b in range(group):
        new_ref[b] = (
            state_ref[b] * decay[i * group + b] + added[b * key_dim : (b + 1) * key_dim, :]
        )

    @pl.when(i == pl.num_programs(0) - 1)
    def _():
        h_ref[...] = (total[...] * gate_ref[...]).astype(BF16)


def retain_packed(decay, side, row, within, qkv, gate, state, block_len):
    batch_size, _, key_dim, value_dim = state.shape
    rows = qkv.shape[0]
    size = within.shape[0]
    group = size // block_len
    whole = lambda *shape: pl.BlockSpec(shape, lambda i: (0,) * len(shape))
    state_spec = pl.BlockSpec((group, key_dim, value_dim), lambda i: (i, 0, 0))
    h, new_state = pl.pallas_call(
        functools.partial(retention_kernel, key_dim, block_len),
        grid=(batch_size // group,),
        out_shape=[
            jax.ShapeDtypeStruct((rows, value_dim), BF16),
            jax.ShapeDtypeStruct((batch_size, key_dim, value_dim), F32),
        ],
        in_specs=[
            pl.BlockSpec(memory_space=pltpu.SMEM),
            pl.BlockSpec((size, side.shape[1]), lambda i: (i, 0)),
            pl.BlockSpec((1, size), lambda i: (0, i)),
            whole(size, size),
            whole(*qkv.shape),
            whole(*gate.shape),
            state_spec,
        ],
        out_specs=[whole(rows, value_dim), state_spec],
        scratch_shapes=[pltpu.VMEM((rows, value_dim), F32)],
        compiler_params=pltpu.CompilerParams(dimension_semantics=("arbitrary",)),
    )(decay, side, row, within, qkv, gate, state.reshape(batch_size, key_dim, value_dim))
    return h, new_state.reshape(state.shape)


class Ring:
    def __init__(self, n, rows, pieces):
        self.n, self.m = n, n // 2
        self.rows, self.pieces = rows, pieces
        self.size = rows // pieces
        me = lax.axis_index("tp")
        self.core = lax.rem(me, 2)
        chip = lax.div(me, 2)
        odd = lax.rem(chip, 2)
        half = lax.div(chip, 2)
        self.pos = (1 - odd) * half + odd * (self.m - 1 - half)
        self.me = me
        self.partner = chip * 2 + 1 - self.core
        self.right = self.device(self.pos + 1)
        self.left = self.device(self.pos - 1)

    def device(self, pos, other=False):
        m = self.m
        pos = lax.rem(pos + m, m)
        far = lax.div(pos, (m + 1) // 2)
        chip = (1 - far) * 2 * pos + far * (2 * (m - 1 - pos) + 1)
        return chip * 2 + (1 - self.core if other else self.core)

    def enter(self):
        barrier = pltpu.get_barrier_semaphore()
        for device in (self.left, self.right, self.partner):
            pl.semaphore_signal(barrier, inc=1, device_id={"tp": device}, device_id_type=MESH)
        pl.semaphore_wait(barrier, 3)

    def piece(self, j):
        return pl.ds(j * self.size, self.size)

    def clockwise(self, j):
        return j < self.pieces // 2

    def to(self, j):
        return self.right if self.clockwise(j) else self.left

    def back(self, j, steps):
        return self.pos - steps if self.clockwise(j) else self.pos + steps

    def order(self):
        half = self.pieces // 2
        return [j for pair in range(half) for j in (pair, pair + half)]


def remote(src, dst, send, recv, device):
    return pltpu.make_async_remote_copy(
        src_ref=src,
        dst_ref=dst,
        send_sem=send,
        recv_sem=recv,
        device_id={"tp": device},
        device_id_type=MESH,
    )


def gather_stage(ring, own_ref, whole, sems):
    width = own_ref.shape[1]
    send, recv, share_send, share_recv = sems

    def columns(device):
        return pl.ds(pl.multiple_of(device * width, width), width)

    whole[:, columns(ring.me)] = own_ref[...]
    hops, shares = {}, []
    for s in range(ring.m):
        for j in ring.order():
            rows = ring.piece(j)
            cols = columns(ring.device(ring.back(j, s)))
            if s > 0:
                hops[j, s - 1].wait_recv()
            src = own_ref.at[rows, :] if s == 0 else whole.at[rows, cols]
            if s < ring.m - 1:
                hop = remote(src, whole.at[rows, cols], send.at[j, s], recv.at[j, s], ring.to(j))
                hop.start()
                hops[j, s] = hop
            share = remote(
                src, whole.at[rows, cols], share_send.at[j, s], share_recv.at[j, s], ring.partner
            )
            share.start()
            shares.append(share)
    for hop in hops.values():
        hop.wait_send()
    for share in shares:
        share.wait()


def fill_weights(wq_ref, wk_ref, wv_ref, wg_ref, wcat):
    at = 0
    for ref in (wq_ref, wk_ref, wv_ref, wg_ref):
        wcat[:, at : at + ref.shape[1]] = ref[...]
        at += ref.shape[1]


def project_stage(whole, gain_ref, wcat, table_ref, qkv_ref, gate_ref, key_dim):
    rows, width = whole.shape
    tile = 16

    @pl.loop(0, rows // tile)
    def _(i):
        at = pl.ds(pl.multiple_of(i * tile, tile), tile)
        x = whole[at, :].astype(F32)
        inv = lax.rsqrt(jnp.mean(x * x, axis=-1, keepdims=True) + NORM_EPSILON)
        whole[at, :] = (x * inv * gain_ref[...]).astype(BF16)

    both = 2 * key_dim
    value_dim = gate_ref.shape[1]
    block = rows // 4

    @pl.loop(0, 4)
    def _(i):
        at = pl.ds(pl.multiple_of(i * block, block), block)
        out = jnp.dot(whole[at, :], wcat[...], preferred_element_type=F32)
        qk = out[:, :both]
        lane = lax.broadcasted_iota(jnp.int32, qk.shape, 1)
        ahead = pltpu.roll(qk, both - key_dim // 2, 1)
        behind = pltpu.roll(qk, key_dim // 2, 1)
        swapped = jnp.where(lax.rem(lane, key_dim) < key_dim // 2, ahead, behind)
        turned = qk * table_ref[at, :both] + swapped * table_ref[at, both:]
        qkv_ref[at, :both] = turned.astype(BF16)
        qkv_ref[at, both:] = out[:, both : both + value_dim].astype(BF16)
        gate = out[:, both + value_dim :]
        gate_ref[at, :] = gate / (1.0 + jnp.exp(-gate))


def scatter_stage(ring, h_ref, w_ref, x_ref, out_ref, h_pair, w_pair, outbox, inbox, sems):
    width = x_ref.shape[1]
    depth = h_ref.shape[1]
    send, recv, pair_send, pair_recv = sems
    w_copy = remote(
        w_ref, w_pair.at[pl.ds(depth, depth), :], pair_send.at[0], pair_recv.at[0], ring.partner
    )
    w_copy.start()
    h_copy = remote(
        h_ref, h_pair.at[:, pl.ds(depth, depth)], pair_send.at[1], pair_recv.at[1], ring.partner
    )
    h_copy.start()
    w_pair[:depth, :] = w_ref[...]
    h_pair[:, :depth] = h_ref[...]
    w_copy.wait()
    h_copy.wait()
    hops = {}
    for s in range(ring.m):
        for j in ring.order():
            rows = ring.piece(j)
            target = ring.device(ring.back(j, s + 1))
            cols = pl.ds(pl.multiple_of(target * width, width), width)
            part = jnp.dot(h_pair[rows, :], w_pair[:, cols], preferred_element_type=F32)
            if s > 0:
                hops[j, s - 1].wait_recv()
                part = part + inbox[j, s - 1].astype(F32)
            if s < ring.m - 1:
                outbox[j, s] = part.astype(BF16)
                hop = remote(
                    outbox.at[j, s], inbox.at[j, s], send.at[j, s], recv.at[j, s], ring.to(j)
                )
                hop.start()
                hops[j, s] = hop
            else:
                mix = part.astype(BF16).astype(F32)
                out_ref[rows, :] = (x_ref[rows, :].astype(F32) + mix).astype(BF16)
    for hop in hops.values():
        hop.wait_send()


def first_kernel(n, pieces, key_dim, *refs):
    x_ref, gain_ref, wq, wk, wv, wg, table, qkv, gate, whole, wcat, *sems = refs
    ring = Ring(n, x_ref.shape[0], pieces)
    ring.enter()
    fill_weights(wq, wk, wv, wg, wcat)
    gather_stage(ring, x_ref, whole, sems)
    project_stage(whole, gain_ref, wcat, table, qkv, gate, key_dim)


def middle_kernel(n, pieces, key_dim, *refs):
    h_ref, w_ref, x_ref, gain_ref, wq, wk, wv, wg, table = refs[:9]
    x1, qkv, gate, whole, wcat, h_pair, w_pair, outbox, inbox = refs[9:18]
    sems = refs[18:]
    ring = Ring(n, x_ref.shape[0], pieces)
    ring.enter()
    fill_weights(wq, wk, wv, wg, wcat)
    scatter_stage(ring, h_ref, w_ref, x_ref, x1, h_pair, w_pair, outbox, inbox, sems[4:])
    gather_stage(ring, x1, whole, sems[:4])
    project_stage(whole, gain_ref, wcat, table, qkv, gate, key_dim)


def last_kernel(n, pieces, *refs):
    h_ref, w_ref, x_ref, out_ref, h_pair, w_pair, outbox, inbox, *sems = refs
    ring = Ring(n, x_ref.shape[0], pieces)
    ring.enter()
    scatter_stage(ring, h_ref, w_ref, x_ref, out_ref, h_pair, w_pair, outbox, inbox, sems)


def gather_scratch(n, pieces, rows, width, wide):
    scratch = [pltpu.VMEM((rows, n * width), BF16), pltpu.VMEM((n * width, wide), BF16)]
    m = n // 2
    sems = [pltpu.SemaphoreType.DMA((pieces, m - 1))] * 2 + [pltpu.SemaphoreType.DMA((pieces, m))] * 2
    return scratch, sems


def scatter_scratch(n, pieces, rows, width, depth):
    m = n // 2
    boxes = pltpu.VMEM((pieces, m - 1, rows // pieces, width), BF16)
    scratch = [
        pltpu.VMEM((rows, 2 * depth), BF16),
        pltpu.VMEM((2 * depth, n * width), BF16),
        boxes,
        boxes,
    ]
    sems = [pltpu.SemaphoreType.DMA((pieces, m - 1))] * 2 + [pltpu.SemaphoreType.DMA((2,))] * 2
    return scratch, sems


def call(kernel, outs, scratch, collective_id, *args):
    vmem = pl.BlockSpec(memory_space=pltpu.VMEM)
    return pl.pallas_call(
        kernel,
        out_shape=outs,
        in_specs=[vmem] * len(args),
        out_specs=[vmem] * len(outs),
        scratch_shapes=scratch,
        compiler_params=pltpu.CompilerParams(
            collective_id=collective_id, has_side_effects=True, vmem_limit_bytes=56 * 2**20
        ),
    )(*args)


def plain_project(x, gain, weights, table, key_dim):
    whole = lax.all_gather(x, "tp", axis=1, tiled=True).astype(F32)
    inv = lax.rsqrt(jnp.mean(whole * whole, axis=-1, keepdims=True) + NORM_EPSILON)
    normed = (whole * inv * gain).astype(BF16)
    qk = jnp.dot(normed, jnp.concatenate(weights[:2], axis=1), preferred_element_type=F32)
    halves = qk.reshape(qk.shape[0], 2, 2, key_dim // 2)
    swapped = halves[:, :, ::-1].reshape(qk.shape)
    turned = qk * table[:, : 2 * key_dim] + swapped * table[:, 2 * key_dim :]
    values = jnp.dot(normed, weights[2], preferred_element_type=F32)
    gate = jnp.dot(normed, weights[3], preferred_element_type=F32)
    qkv = jnp.concatenate([turned.astype(BF16), values.astype(BF16)], axis=1)
    return qkv, jax.nn.silu(gate)


def plain_finish(h, w_out, x):
    part = jnp.dot(h, w_out, preferred_element_type=F32).astype(BF16)
    mix = lax.psum_scatter(part, "tp", scatter_dimension=1, tiled=True)
    return (x.astype(F32) + mix.astype(F32)).astype(BF16)


def shards(
    tokens,
    lengths,
    gain_first,
    query_first,
    key_first,
    value_first,
    gate_first,
    out_first,
    state_first,
    gain_second,
    query_second,
    key_second,
    value_second,
    gate_second,
    out_second,
    state_second,
):
    n = lax.axis_size("tp")
    batch_size, head_count, key_dim, value_dim = state_first.shape
    slots, width = tokens.shape
    block_len = slots // batch_size
    rows = LIVE_TOTAL

    lengths_i = lengths.astype(jnp.int32)
    starts = jnp.cumsum(lengths_i) - lengths_i
    slot = jnp.arange(block_len, dtype=jnp.int32)
    live = slot[None, :] < lengths_i[:, None]
    target = jnp.where(live, starts[:, None] + slot[None, :], -1).reshape(slots)
    pack = (jnp.arange(rows, dtype=jnp.int32)[:, None] == target[None, :]).astype(BF16)

    def packed(padded):
        return jnp.dot(pack, padded, preferred_element_type=F32)

    def spread(rows_in):
        return lax.dot_general(
            pack, rows_in, (((0,), (0,)), ((), ())), preferred_element_type=F32
        ).astype(rows_in.dtype)

    slot_hot = jnp.tile(jnp.eye(block_len, dtype=BF16), (batch_size, 1))
    table = jnp.dot(
        packed(slot_hot), rope_tables(block_len, key_dim), precision=lax.Precision.HIGHEST
    )
    x = packed(tokens).astype(BF16)

    weights_first = (query_first, key_first, value_first, gate_first)
    weights_second = (query_second, key_second, value_second, gate_second)
    wide = sum(w.shape[1] for w in weights_first)
    pieces = next((p for p in (6, 4, 2) if rows % (16 * p) == 0), 0)
    ringed = (
        n >= 4
        and n % 2 == 0
        and pieces > 0
        and rows % 64 == 0
        and head_count == 1
        and width % 128 == 0
        and value_dim % 128 == 0
        and 2 * key_dim % 128 == 0
    )
    size = 128
    grouped = (
        head_count == 1
        and size % (2 * block_len) == 0
        and slots % size == 0
        and 2 * key_dim == 128
        and value_dim % 128 == 0
        and rows % 16 == 0
    )
    if grouped:
        log_gamma = decay_logs(1)[0]
        slot_f, count = slot.astype(F32), lengths_i.astype(F32)
        inward = jnp.broadcast_to(jnp.exp(log_gamma * (slot_f + 1.0))[None, :], live.shape)
        gap = jnp.maximum(count[:, None] - 1.0 - slot_f[None, :], 0.0)
        onward = jnp.exp(log_gamma * gap)
        side = jnp.stack([target.astype(F32), inward.reshape(slots), onward.reshape(slots)], axis=1)
        decay = jnp.exp(log_gamma * count)
        r = jnp.arange(size, dtype=jnp.int32)
        step = (r[:, None] - r[None, :]).astype(F32)
        same = (r[:, None] // block_len == r[None, :] // block_len) & (step >= 0.0)
        within = jnp.where(same, jnp.exp(log_gamma * jnp.maximum(step, 0.0)), 0.0)

    def retention(qkv, gate, state):
        if grouped:
            return retain_packed(
                decay, side, target[None, :], within, qkv, gate, state, block_len
            )
        normed, new_state = retain(spread(qkv), lengths, state)
        return (packed(normed) * gate).astype(BF16), new_state

    outs = [
        jax.ShapeDtypeStruct((rows, 2 * key_dim + value_dim), BF16),
        jax.ShapeDtypeStruct((rows, value_dim), F32),
    ]
    own = jax.ShapeDtypeStruct((rows, width), BF16)
    gather_bufs, gather_sems = gather_scratch(n, pieces or 2, rows, width, wide)
    scatter_bufs, scatter_sems = scatter_scratch(n, pieces or 2, rows, width, value_dim)

    if ringed:
        qkv, gate = call(
            functools.partial(first_kernel, n, pieces, key_dim),
            outs,
            gather_bufs + gather_sems,
            0,
            x,
            gain_first[None],
            *weights_first,
            table,
        )
    else:
        qkv, gate = plain_project(x, gain_first, weights_first, table, key_dim)
    h, state_first_new = retention(qkv, gate, state_first)
    if ringed:
        x1, qkv, gate = call(
            functools.partial(middle_kernel, n, pieces, key_dim),
            [own] + outs,
            gather_bufs + scatter_bufs + gather_sems + scatter_sems,
            1,
            h,
            out_first,
            x,
            gain_second[None],
            *weights_second,
            table,
        )
    else:
        x1 = plain_finish(h, out_first, x)
        qkv, gate = plain_project(x1, gain_second, weights_second, table, key_dim)
    h, state_second_new = retention(qkv, gate, state_second)
    if ringed:
        (y,) = call(
            functools.partial(last_kernel, n, pieces),
            [own],
            scatter_bufs + scatter_sems,
            2,
            h,
            out_second,
            x1,
        )
    else:
        y = plain_finish(h, out_second, x1)
    mixed_out = jnp.where(live.reshape(slots, 1), spread(y), tokens)
    return (mixed_out, state_first_new, state_second_new)


def solution(mesh):
    heads = P(None, "tp")
    state = P("grp", "tp", None, None)
    block = (P(), heads, heads, heads, heads, P("tp", None), state)
    in_specs = (P("grp", "tp"), P("grp")) + block + block
    out_specs = (P("grp", "tp"), state, state)
    return jax.shard_map(shards, mesh=mesh, in_specs=in_specs, out_specs=out_specs, check_vma=False)
```

```python
import functools

import jax
import jax.numpy as jnp
from jax import lax
from jax.experimental import pallas as pl
from jax.experimental.pallas import tpu as pltpu
from jax.sharding import PartitionSpec as P

PAST_LEN = 16384
LIVE_TOTAL = 960

NORM_EPSILON = 1e-06
ROPE_BASE = 10000.0

MESH = pl.DeviceIdType.MESH
F32 = jnp.float32
BF16 = jnp.bfloat16


def decay_logs(head_count):
    head_total = lax.axis_size("tp") * head_count
    head_ids = (lax.axis_index("tp") * head_count + jnp.arange(head_count)).astype(F32)
    return jnp.log(1.0 - 2.0 ** (-1.5 - 6.0 * head_ids / (head_total - 1)))


def rope_tables(block_len, key_dim):
    half_dim = key_dim // 2
    inverse = ROPE_BASE ** (-jnp.arange(half_dim, dtype=F32) / half_dim)
    positions = PAST_LEN + jnp.arange(block_len, dtype=F32)
    angles = positions[:, None] * inverse[None, :]
    cosines, sines = jnp.cos(angles), jnp.sin(angles)
    cosines = jnp.concatenate([cosines, cosines], axis=1)
    sines = jnp.concatenate([-sines, sines], axis=1)
    scale = key_dim ** (-0.5)
    return jnp.concatenate([cosines, cosines * scale, sines, sines * scale], axis=1)


def retain(qkv, lengths, state_in):
    batch_size, head_count, key_dim, value_dim = state_in.shape
    block_len = qkv.shape[0] // batch_size
    log_gamma = decay_logs(head_count)
    queries = qkv[:, :key_dim].reshape(batch_size, block_len, 1, key_dim)
    key_rows = qkv[:, key_dim : 2 * key_dim].reshape(batch_size, block_len, 1, key_dim)
    values = qkv[:, 2 * key_dim :].reshape(batch_size, block_len, 1, value_dim)
    slot_ids = jnp.arange(block_len).astype(F32)
    live_count = lengths.astype(F32)
    active = (slot_ids[None, :] < live_count[:, None]).astype(F32)
    step_gap = slot_ids[:, None] - slot_ids[None, :]
    causal = (step_gap >= 0.0).astype(F32)
    within = jnp.exp(log_gamma[:, None, None] * jnp.maximum(step_gap, 0.0)[None]) * causal[None]
    scores = jnp.einsum("bihd,bjhd->bhij", queries, key_rows, preferred_element_type=F32)
    weights = (scores * within[None]).astype(BF16)
    inner_part = jnp.einsum("bhij,bjhe->bihe", weights, values, preferred_element_type=F32)
    carried = jnp.einsum(
        "bihd,bhde->bihe", queries.astype(F32), state_in, precision=lax.Precision.HIGHEST
    )
    carried = (
        carried * jnp.exp(log_gamma[None, None, :] * (slot_ids[None, :, None] + 1.0))[..., None]
    )
    retained = (inner_part + carried) * active[:, :, None, None]
    lead_gap = live_count[:, None] - 1.0 - slot_ids[None, :]
    key_weight = (
        jnp.exp(log_gamma[None, None, :] * jnp.maximum(lead_gap, 0.0)[:, :, None])
        * active[:, :, None]
    )
    added_state = jnp.einsum(
        "bjhd,bjhe->bhde",
        key_rows.astype(F32) * key_weight[..., None],
        values.astype(F32),
        precision=lax.Precision.HIGHEST,
    )
    new_state = (
        state_in * jnp.exp(log_gamma[None, :] * live_count[:, None])[:, :, None, None] + added_state
    )
    inv_rms = lax.rsqrt(jnp.mean(retained * retained, axis=-1, keepdims=True) + NORM_EPSILON)
    normed = (retained * inv_rms).astype(BF16)
    return normed.reshape(batch_size * block_len, value_dim), new_state


def retention_kernel(key_dim, block_len, *refs):
    decay, side_ref, row_ref, within_ref, qkv_ref, gate_ref, state_ref = refs[:7]
    h_ref, new_ref, total = refs[7:]
    i = pl.program_id(0)
    rows = qkv_ref.shape[0]
    both = 2 * key_dim
    size = side_ref.shape[0]
    side = side_ref[...]
    unit = within_ref.shape[0]
    group = unit // block_len

    slots = lax.broadcasted_iota(jnp.int32, (size, rows), 1)
    hot = jnp.where(slots == side[:, 0:1].astype(jnp.int32), 1.0, 0.0).astype(BF16)
    padded = jnp.dot(hot, qkv_ref[...], preferred_element_type=F32)
    wide = (unit, group * key_dim)
    own = lax.div(lax.broadcasted_iota(jnp.int32, wide, 0), block_len) == lax.div(
        lax.broadcasted_iota(jnp.int32, wide, 1), key_dim
    )
    front = lax.broadcasted_iota(jnp.int32, (unit, both), 1) < key_dim

    def per_sequence(doubled):
        spread = jnp.concatenate([doubled] * (group // 2), axis=1)
        return jnp.where(own, spread, 0.0).astype(BF16)

    def one(u):
        at = slice(u * unit, (u + 1) * unit)
        first = u * group
        qk, values = padded[at, :both], padded[at, both:].astype(BF16)
        turned = pltpu.roll(qk, key_dim, 1)
        queries, keys = jnp.where(front, qk, turned), jnp.where(front, turned, qk)
        scores = lax.dot_general(
            jnp.where(front, qk, 0.0).astype(BF16),
            keys.astype(BF16),
            (((1,), (1,)), ((), ())),
            preferred_element_type=F32,
        )
        weights = (scores * within_ref[...]).astype(BF16)
        retained = jnp.dot(weights, values, preferred_element_type=F32)
        state = state_ref[first : first + group].reshape(group * key_dim, state_ref.shape[-1])
        high = state.astype(BF16)
        low = (state - high.astype(F32)).astype(BF16)
        wide_q = per_sequence(queries)
        carried = jnp.dot(wide_q, high, preferred_element_type=F32)
        carried = carried + jnp.dot(wide_q, low, preferred_element_type=F32)
        retained = retained + carried * side[at, 1:2]
        inv = lax.rsqrt(jnp.mean(retained * retained, axis=-1, keepdims=True) + NORM_EPSILON)

        scaled = keys * side[at, 2:3]
        k_high = scaled.astype(BF16).astype(F32)
        added = None
        for piece in (k_high, scaled - k_high):
            term = lax.dot_general(
                per_sequence(piece), values, (((0,), (0,)), ((), ())), preferred_element_type=F32
            )
            added = term if added is None else added + term
        for b in range(group):
            new_ref[first + b] = (
                state_ref[first + b] * decay[i * (size // block_len) + first + b]
                + added[b * key_dim : (b + 1) * key_dim, :]
            )
        return (retained * inv).astype(BF16)

    normed = jnp.concatenate([one(u) for u in range(size // unit)], axis=0)
    places = lax.broadcasted_iota(jnp.int32, (rows, size), 0)
    back = jnp.where(places == row_ref[...], 1.0, 0.0).astype(BF16)
    part = jnp.dot(back, normed, preferred_element_type=F32)

    @pl.when(i == 0)
    def _():
        total[...] = part

    @pl.when(i > 0)
    def _():
        total[...] += part

    @pl.when(i == pl.num_programs(0) - 1)
    def _():
        h_ref[...] = (total[...] * gate_ref[...]).astype(BF16)


def retain_packed(decay, side, row, within, qkv, gate, state, block_len):
    batch_size, _, key_dim, value_dim = state.shape
    rows = qkv.shape[0]
    unit = within.shape[0]
    many = next(k for k in (3, 2, 1) if batch_size * block_len % (k * unit) == 0)
    size = many * unit
    group = size // block_len
    whole = lambda *shape: pl.BlockSpec(shape, lambda i: (0,) * len(shape))
    state_spec = pl.BlockSpec((group, key_dim, value_dim), lambda i: (i, 0, 0))
    h, new_state = pl.pallas_call(
        functools.partial(retention_kernel, key_dim, block_len),
        grid=(batch_size // group,),
        out_shape=[
            jax.ShapeDtypeStruct((rows, value_dim), BF16),
            jax.ShapeDtypeStruct((batch_size, key_dim, value_dim), F32),
        ],
        in_specs=[
            pl.BlockSpec(memory_space=pltpu.SMEM),
            pl.BlockSpec((size, side.shape[1]), lambda i: (i, 0)),
            pl.BlockSpec((1, size), lambda i: (0, i)),
            whole(unit, unit),
            whole(*qkv.shape),
            whole(*gate.shape),
            state_spec,
        ],
        out_specs=[whole(rows, value_dim), state_spec],
        scratch_shapes=[pltpu.VMEM((rows, value_dim), F32)],
        compiler_params=pltpu.CompilerParams(dimension_semantics=("arbitrary",)),
    )(decay, side, row, within, qkv, gate, state.reshape(batch_size, key_dim, value_dim))
    return h, new_state.reshape(state.shape)


class Ring:
    def __init__(self, n, rows, pieces):
        self.n, self.m = n, n // 2
        self.rows, self.pieces = rows, pieces
        self.size = rows // pieces
        me = lax.axis_index("tp")
        self.core = lax.rem(me, 2)
        chip = lax.div(me, 2)
        odd = lax.rem(chip, 2)
        half = lax.div(chip, 2)
        self.pos = (1 - odd) * half + odd * (self.m - 1 - half)
        self.me = me
        self.partner = chip * 2 + 1 - self.core
        self.right = self.device(self.pos + 1)
        self.left = self.device(self.pos - 1)

    def device(self, pos, other=False):
        m = self.m
        pos = lax.rem(pos + m, m)
        far = lax.div(pos, (m + 1) // 2)
        chip = (1 - far) * 2 * pos + far * (2 * (m - 1 - pos) + 1)
        return chip * 2 + (1 - self.core if other else self.core)

    def enter(self):
        barrier = pltpu.get_barrier_semaphore()
        for device in (self.left, self.right, self.partner):
            pl.semaphore_signal(barrier, inc=1, device_id={"tp": device}, device_id_type=MESH)
        pl.semaphore_wait(barrier, 3)

    def piece(self, j):
        return pl.ds(j * self.size, self.size)

    def clockwise(self, j):
        return j < self.pieces // 2

    def to(self, j):
        return self.right if self.clockwise(j) else self.left

    def back(self, j, steps):
        return self.pos - steps if self.clockwise(j) else self.pos + steps

    def order(self):
        half = self.pieces // 2
        return [j for pair in range(half) for j in (pair, pair + half)]


def remote(src, dst, send, recv, device):
    return pltpu.make_async_remote_copy(
        src_ref=src,
        dst_ref=dst,
        send_sem=send,
        recv_sem=recv,
        device_id={"tp": device},
        device_id_type=MESH,
    )


def gather_stage(ring, own_ref, whole, sems, prepare, consume):
    width = own_ref.shape[1]
    send, recv, share_send, share_recv = sems

    def columns(device):
        return pl.ds(pl.multiple_of(device * width, width), width)

    hops, shares = {}, {}

    def use(s):
        for j in range(ring.pieces):
            shares[j, s].wait_recv()
        for way in (0, ring.pieces // 2):
            chip = lax.div(ring.device(ring.back(way, s)), 2)
            consume(way * ring.size, chip)

    for s in range(ring.m):
        for j in ring.order():
            rows = ring.piece(j)
            cols = columns(ring.device(ring.back(j, s)))
            if s > 0:
                hops[j, s - 1].wait_recv()
            src = own_ref.at[rows, :] if s == 0 else whole.at[rows, cols]
            if s < ring.m - 1:
                hop = remote(src, whole.at[rows, cols], send.at[j, s], recv.at[j, s], ring.to(j))
                hop.start()
                hops[j, s] = hop
            share = remote(
                src, whole.at[rows, cols], share_send.at[j, s], share_recv.at[j, s], ring.partner
            )
            share.start()
            shares[j, s] = share
        if s == 0:
            whole[:, columns(ring.me)] = own_ref[...]
            prepare()
        else:
            use(s - 1)
    use(ring.m - 1)
    for hop in hops.values():
        hop.wait_send()
    for share in shares.values():
        share.wait_send()


def fill_weights(wq_ref, wk_ref, wv_ref, wg_ref, wcat, total, squares):
    both = 2 * wq_ref.shape[0]
    step = 128

    @pl.loop(0, wcat.shape[0] // step)
    def _(i):
        at = pl.ds(pl.multiple_of(i * step, step), step)
        pair = jnp.concatenate([wq_ref[:, at], wk_ref[:, at]], axis=0)
        wcat[at, :both] = jnp.transpose(pair.astype(F32)).astype(BF16)

    mid = both + wv_ref.shape[1]
    wcat[:, both:mid] = wv_ref[...]
    wcat[:, mid:] = wg_ref[...]
    total[...] = jnp.zeros_like(total)
    squares[...] = jnp.zeros_like(squares)


def consumer(whole, width, gain_ref, wcat, total, squares):
    half = whole.shape[0] // 2
    block = half // 2

    def consume(first, chip):
        cols = pl.ds(pl.multiple_of(chip * 2 * width, 2 * width), 2 * width)
        gain = gain_ref[:, cols]

        @pl.loop(0, 2)
        def _(i):
            at = pl.ds(pl.multiple_of(first + i * block, 16), block)
            x = whole[at, cols].astype(F32)
            square = x * x
            part = square[:, :128]
            for k in range(128, 2 * width, 128):
                part = part + square[:, k : k + 128]
            squares[at, :] += part
            total[at, :] += jnp.dot(
                (x * gain).astype(BF16), wcat[cols, :], preferred_element_type=F32
            )

    return consume


def project_stage(width, total, squares, table_ref, qkv_ref, gate_ref, key_dim):
    rows = total.shape[0]
    both = 2 * key_dim
    value_dim = gate_ref.shape[1]
    block = rows // 4

    @pl.loop(0, 4)
    def _(i):
        at = pl.ds(pl.multiple_of(i * block, block), block)
        mean = jnp.sum(squares[at, :], axis=-1, keepdims=True) / width
        out = total[at, :] * lax.rsqrt(mean + NORM_EPSILON)
        qk = out[:, :both]
        lane = lax.broadcasted_iota(jnp.int32, qk.shape, 1)
        ahead = pltpu.roll(qk, both - key_dim // 2, 1)
        behind = pltpu.roll(qk, key_dim // 2, 1)
        swapped = jnp.where(lax.rem(lane, key_dim) < key_dim // 2, ahead, behind)
        turned = qk * table_ref[at, :both] + swapped * table_ref[at, both:]
        qkv_ref[at, :both] = turned.astype(BF16)
        qkv_ref[at, both:] = out[:, both : both + value_dim].astype(BF16)
        gate = out[:, both + value_dim :]
        gate_ref[at, :] = gate / (1.0 + jnp.exp(-gate))


def scatter_stage(ring, h_ref, w_ref, x_ref, out_ref, h_pair, w_pair, outbox, inbox, sems, prepare):
    width = x_ref.shape[1]
    depth = h_ref.shape[1]
    send, recv, pair_send, pair_recv = sems
    w_copy = remote(
        w_ref, w_pair.at[pl.ds(depth, depth), :], pair_send.at[0], pair_recv.at[0], ring.partner
    )
    w_copy.start()
    h_copy = remote(
        h_ref, h_pair.at[:, pl.ds(depth, depth)], pair_send.at[1], pair_recv.at[1], ring.partner
    )
    h_copy.start()
    prepare()
    w_pair[:depth, :] = w_ref[...]
    h_pair[:, :depth] = h_ref[...]
    w_copy.wait()
    h_copy.wait()
    hops = {}
    for s in range(ring.m):
        for j in ring.order():
            rows = ring.piece(j)
            target = ring.device(ring.back(j, s + 1))
            cols = pl.ds(pl.multiple_of(target * width, width), width)
            part = jnp.dot(h_pair[rows, :], w_pair[:, cols], preferred_element_type=F32)
            if s > 0:
                hops[j, s - 1].wait_recv()
                part = part + inbox[j, s - 1].astype(F32)
            if s < ring.m - 1:
                outbox[j, s] = part.astype(BF16)
                hop = remote(
                    outbox.at[j, s], inbox.at[j, s], send.at[j, s], recv.at[j, s], ring.to(j)
                )
                hop.start()
                hops[j, s] = hop
            else:
                mix = part.astype(BF16).astype(F32)
                out_ref[rows, :] = (x_ref[rows, :].astype(F32) + mix).astype(BF16)
    for hop in hops.values():
        hop.wait_send()


def nothing():
    pass


def first_kernel(n, pieces, key_dim, *refs):
    x_ref, gain_ref, wq, wk, wv, wg, table, qkv, gate, whole, wcat, total, squares, *sems = refs
    ring = Ring(n, x_ref.shape[0], pieces)
    ring.enter()
    fill = functools.partial(fill_weights, wq, wk, wv, wg, wcat, total, squares)
    consume = consumer(whole, x_ref.shape[1], gain_ref, wcat, total, squares)
    gather_stage(ring, x_ref, whole, sems, fill, consume)
    project_stage(whole.shape[1], total, squares, table, qkv, gate, key_dim)


def middle_kernel(n, pieces, key_dim, *refs):
    h_ref, w_ref, x_ref, gain_ref, wq, wk, wv, wg, table = refs[:9]
    x1, qkv, gate, whole, wcat, total, squares, h_pair, w_pair, outbox, inbox = refs[9:20]
    sems = refs[20:]
    ring = Ring(n, x_ref.shape[0], pieces)
    ring.enter()
    fill = functools.partial(fill_weights, wq, wk, wv, wg, wcat, total, squares)
    consume = consumer(whole, x_ref.shape[1], gain_ref, wcat, total, squares)
    scatter_stage(
        ring, h_ref, w_ref, x_ref, x1, h_pair, w_pair, outbox, inbox, sems[4:], fill
    )
    gather_stage(ring, x1, whole, sems[:4], nothing, consume)
    project_stage(whole.shape[1], total, squares, table, qkv, gate, key_dim)


def last_kernel(n, pieces, *refs):
    h_ref, w_ref, x_ref, out_ref, h_pair, w_pair, outbox, inbox, *sems = refs
    ring = Ring(n, x_ref.shape[0], pieces)
    ring.enter()
    scatter_stage(
        ring, h_ref, w_ref, x_ref, out_ref, h_pair, w_pair, outbox, inbox, sems, nothing
    )


def gather_scratch(n, pieces, rows, width, wide):
    scratch = [
        pltpu.VMEM((rows, n * width), BF16),
        pltpu.VMEM((n * width, wide), BF16),
        pltpu.VMEM((rows, wide), F32),
        pltpu.VMEM((rows, 128), F32),
    ]
    m = n // 2
    sems = [pltpu.SemaphoreType.DMA((pieces, m - 1))] * 2 + [pltpu.SemaphoreType.DMA((pieces, m))] * 2
    return scratch, sems


def scatter_scratch(n, pieces, rows, width, depth):
    m = n // 2
    boxes = pltpu.VMEM((pieces, m - 1, rows // pieces, width), BF16)
    scratch = [
        pltpu.VMEM((rows, 2 * depth), BF16),
        pltpu.VMEM((2 * depth, n * width), BF16),
        boxes,
        boxes,
    ]
    sems = [pltpu.SemaphoreType.DMA((pieces, m - 1))] * 2 + [pltpu.SemaphoreType.DMA((2,))] * 2
    return scratch, sems


def call(kernel, outs, scratch, collective_id, *args):
    vmem = pl.BlockSpec(memory_space=pltpu.VMEM)
    return pl.pallas_call(
        kernel,
        out_shape=outs,
        in_specs=[vmem] * len(args),
        out_specs=[vmem] * len(outs),
        scratch_shapes=scratch,
        compiler_params=pltpu.CompilerParams(
            collective_id=collective_id, has_side_effects=True, vmem_limit_bytes=56 * 2**20
        ),
    )(*args)


def plain_project(x, gain, weights, table, key_dim):
    whole = lax.all_gather(x, "tp", axis=1, tiled=True).astype(F32)
    inv = lax.rsqrt(jnp.mean(whole * whole, axis=-1, keepdims=True) + NORM_EPSILON)
    normed = (whole * inv * gain).astype(BF16)
    qk = jnp.dot(normed, jnp.concatenate(weights[:2], axis=1), preferred_element_type=F32)
    halves = qk.reshape(qk.shape[0], 2, 2, key_dim // 2)
    swapped = halves[:, :, ::-1].reshape(qk.shape)
    turned = qk * table[:, : 2 * key_dim] + swapped * table[:, 2 * key_dim :]
    values = jnp.dot(normed, weights[2], preferred_element_type=F32)
    gate = jnp.dot(normed, weights[3], preferred_element_type=F32)
    qkv = jnp.concatenate([turned.astype(BF16), values.astype(BF16)], axis=1)
    return qkv, jax.nn.silu(gate)


def plain_finish(h, w_out, x):
    part = jnp.dot(h, w_out, preferred_element_type=F32).astype(BF16)
    mix = lax.psum_scatter(part, "tp", scatter_dimension=1, tiled=True)
    return (x.astype(F32) + mix.astype(F32)).astype(BF16)


def shards(
    tokens,
    lengths,
    gain_first,
    query_first,
    key_first,
    value_first,
    gate_first,
    out_first,
    state_first,
    gain_second,
    query_second,
    key_second,
    value_second,
    gate_second,
    out_second,
    state_second,
):
    n = lax.axis_size("tp")
    batch_size, head_count, key_dim, value_dim = state_first.shape
    slots, width = tokens.shape
    block_len = slots // batch_size
    rows = LIVE_TOTAL

    lengths_i = lengths.astype(jnp.int32)
    starts = jnp.cumsum(lengths_i) - lengths_i
    slot = jnp.arange(block_len, dtype=jnp.int32)
    live = slot[None, :] < lengths_i[:, None]
    target = jnp.where(live, starts[:, None] + slot[None, :], -1).reshape(slots)
    pack = (jnp.arange(rows, dtype=jnp.int32)[:, None] == target[None, :]).astype(BF16)

    def packed(padded):
        return jnp.dot(pack, padded, preferred_element_type=F32)

    def spread(rows_in):
        return lax.dot_general(
            pack, rows_in, (((0,), (0,)), ((), ())), preferred_element_type=F32
        ).astype(rows_in.dtype)

    slot_hot = jnp.tile(jnp.eye(block_len, dtype=BF16), (batch_size, 1))
    table = jnp.dot(
        packed(slot_hot), rope_tables(block_len, key_dim), precision=lax.Precision.HIGHEST
    )
    x = packed(tokens).astype(BF16)

    weights_first = (query_first, key_first, value_first, gate_first)
    weights_second = (query_second, key_second, value_second, gate_second)
    wide = sum(w.shape[1] for w in weights_first)
    pieces = next((p for p in (10, 6, 4, 2) if rows % (16 * p) == 0), 0)
    ringed = (
        n >= 4
        and n % 2 == 0
        and pieces > 0
        and rows % 64 == 0
        and head_count == 1
        and width % 128 == 0
        and value_dim % 128 == 0
        and 2 * key_dim % 128 == 0
    )
    size = 128
    grouped = (
        head_count == 1
        and size % (2 * block_len) == 0
        and slots % size == 0
        and 2 * key_dim == 128
        and value_dim % 128 == 0
        and rows % 16 == 0
    )
    if grouped:
        log_gamma = decay_logs(1)[0]
        slot_f, count = slot.astype(F32), lengths_i.astype(F32)
        inward = jnp.broadcast_to(jnp.exp(log_gamma * (slot_f + 1.0))[None, :], live.shape)
        gap = jnp.maximum(count[:, None] - 1.0 - slot_f[None, :], 0.0)
        onward = jnp.exp(log_gamma * gap)
        side = jnp.stack([target.astype(F32), inward.reshape(slots), onward.reshape(slots)], axis=1)
        decay = jnp.exp(log_gamma * count)
        r = jnp.arange(size, dtype=jnp.int32)
        step = (r[:, None] - r[None, :]).astype(F32)
        same = (r[:, None] // block_len == r[None, :] // block_len) & (step >= 0.0)
        within = jnp.where(same, jnp.exp(log_gamma * jnp.maximum(step, 0.0)), 0.0)

    def retention(qkv, gate, state):
        if grouped:
            return retain_packed(
                decay, side, target[None, :], within, qkv, gate, state, block_len
            )
        normed, new_state = retain(spread(qkv), lengths, state)
        return (packed(normed) * gate).astype(BF16), new_state

    outs = [
        jax.ShapeDtypeStruct((rows, 2 * key_dim + value_dim), BF16),
        jax.ShapeDtypeStruct((rows, value_dim), F32),
    ]
    own = jax.ShapeDtypeStruct((rows, width), BF16)
    gather_bufs, gather_sems = gather_scratch(n, pieces or 2, rows, width, wide)
    scatter_bufs, scatter_sems = scatter_scratch(n, pieces or 2, rows, width, value_dim)

    def turned(weights):
        return (weights[0].T, weights[1].T) + weights[2:]

    if ringed:
        qkv, gate = call(
            functools.partial(first_kernel, n, pieces, key_dim),
            outs,
            gather_bufs + gather_sems,
            0,
            x,
            gain_first[None],
            *turned(weights_first),
            table,
        )
    else:
        qkv, gate = plain_project(x, gain_first, weights_first, table, key_dim)
    h, state_first_new = retention(qkv, gate, state_first)
    if ringed:
        x1, qkv, gate = call(
            functools.partial(middle_kernel, n, pieces, key_dim),
            [own] + outs,
            gather_bufs + scatter_bufs + gather_sems + scatter_sems,
            1,
            h,
            out_first,
            x,
            gain_second[None],
            *turned(weights_second),
            table,
        )
    else:
        x1 = plain_finish(h, out_first, x)
        qkv, gate = plain_project(x1, gain_second, weights_second, table, key_dim)
    h, state_second_new = retention(qkv, gate, state_second)
    if ringed:
        (y,) = call(
            functools.partial(last_kernel, n, pieces),
            [own],
            scatter_bufs + scatter_sems,
            2,
            h,
            out_second,
            x1,
        )
    else:
        y = plain_finish(h, out_second, x1)
    mixed_out = jnp.where(live.reshape(slots, 1), spread(y), tokens)
    return (mixed_out, state_first_new, state_second_new)


def solution(mesh):
    heads = P(None, "tp")
    state = P("grp", "tp", None, None)
    block = (P(), heads, heads, heads, heads, P("tp", None), state)
    in_specs = (P("grp", "tp"), P("grp")) + block + block
    out_specs = (P("grp", "tp"), state, state)
    return jax.shard_map(shards, mesh=mesh, in_specs=in_specs, out_specs=out_specs, check_vma=False)
```
